32 devices in a mesh: sp: 8 (over z, y), tp: 4 (over x, core).
Axes of the slice: x: 2, y: 2, z: 4, core: 2. Of those that a mesh axis runs over, the one named last changes fastest.
Arguments:
- target: bfloat16 [2048, 2048], P(('sp', 'tp')), may hold values from -6 to 6
- source: bfloat16 [4096, 2048], P(('sp', 'tp')), may hold values from -6 to 6
- target_gain: bfloat16 [2, 2048], replicated, may hold values from 0.099609375 to 1.8984375
- source_gain: bfloat16 [2, 2048], replicated, may hold values from 0.099609375 to 1.8984375
- query_w: bfloat16 [2, 2048, 8192], P(None, None, 'tp'), may hold values from -0.125 to 0.125
- key_w: bfloat16 [2, 2048, 4096], P(None, None, 'tp'), may hold values from -0.125 to 0.125
- value_w: bfloat16 [2, 2048, 4096], P(None, None, 'tp'), may hold values from -0.125 to 0.125
- out_w: bfloat16 [2, 8192, 2048], P(None, 'tp'), may hold values from -0.1875 to 0.1875
- head_temp: float32 [2, 16], P(None, 'tp'), may hold values from 1.5 to 8, as said below
- final_gain: bfloat16 [2048], replicated, may hold values from 0.099609375 to 1.8984375
Outputs:
- result: float32 [2048, 2048], P(('sp', 'tp'))
The draws below stay inside these ranges and needn't reach their ends.
Inputs may be any that keep to these rules, and one draw needn't show every extreme that they name: `head_temp`: a positive scale for each head's scores.
All inputs are finite; a program needn't handle non-finite values.
Results may differ from the reference program's by a relative error of at most 0.04.
Values may be sent and summed in bfloat16 or wider, within the bound.
No kernel may reach another device: no remote copies, remote signals or barrier semaphores. Data moves between devices by JAX's collectives and lax.ppermute only.
A program may use at most 192 MiB of HBM per device.

```python
import math
import jax
import jax.numpy as jnp
from jax import lax

D = 2048
HEAD_DIM = 512
HEADS = 16
KV_HEADS = 8
SOURCE = 4096
TARGET = 2048
N_TP = 4


def draw_head_temp(key, part):
    moderate_key = jax.random.fold_in(key, 11)
    moderate = jnp.exp(jax.random.uniform(moderate_key, (2, HEADS), jnp.float32, math.log(1.5), math.log(3.5)))
    return moderate


def block_scale(stream_key, extent, cuts, smallest, high):
    level = 1.0
    for position, parts in cuts:
        draws = jax.random.uniform(jax.random.fold_in(jax.random.fold_in(stream_key, 6), position), (parts,), jnp.float32, smallest / len(cuts), high / len(cuts))
        level = level * jnp.repeat(jnp.exp(draws), extent[position] // parts).reshape((-1,) + (1,) * (len(extent) - 1 - position))
    return level


def noise(rng, extent, width, bound, cuts=(), kind=jnp.bfloat16):
    factor_of = block_scale(rng, extent, cuts, -0.22, 0.18) if cuts else 1.0
    array = jax.random.normal(rng, extent, jnp.float32) * width * factor_of
    return jnp.minimum(jnp.maximum(array, -bound), bound).astype(kind)


def setup_inputs(seed: int = 0) -> dict:
    splits = jax.random.split(jax.random.key(seed), 11)
    target = noise(splits[0], (TARGET, D), 1.0, 6.0, ((0, 32),))
    source = noise(splits[1], (SOURCE, D), 1.0, 6.0, ((0, 32),))
    target_gain = jnp.clip(1.0 + 0.18 * jax.random.normal(splits[2], (2, D), jnp.float32), 0.099609375, 1.8984375).astype(jnp.bfloat16)
    source_gain = jnp.clip(1.0 + 0.18 * jax.random.normal(splits[3], (2, D), jnp.float32), 0.099609375, 1.8984375).astype(jnp.bfloat16)
    query_w = noise(splits[4], (2, D, HEADS * HEAD_DIM), D ** -0.5, 0.125, ((2, 4),))
    key_w = noise(splits[5], (2, D, KV_HEADS * HEAD_DIM), D ** -0.5, 0.125, ((2, 4),))
    value_w = noise(splits[6], (2, D, KV_HEADS * HEAD_DIM), D ** -0.5, 0.125, ((2, 4),))
    out_w = noise(splits[7], (2, HEADS * HEAD_DIM, D), (3.0 * (HEADS * HEAD_DIM) ** -0.5), 0.1875, ((1, 4),))
    head_temp = draw_head_temp(jax.random.fold_in(splits[10], 71), 0)
    final_gain = jnp.clip(1.0 + 0.18 * jax.random.normal(splits[9], (D,), jnp.float32), 0.099609375, 1.8984375).astype(jnp.bfloat16)
    return dict(target=target, source=source, target_gain=target_gain, source_gain=source_gain, query_w=query_w, key_w=key_w, value_w=value_w, out_w=out_w, head_temp=head_temp, final_gain=final_gain)


EPS = 1e-06

def unit_rows(matrix):
    values = matrix.astype(jnp.float32)
    return values * lax.rsqrt(lax.optimization_barrier(jnp.mean(values * values, axis=-1, keepdims=True)) + EPS)

def attend_head(queries, key_rows, value_rows, scales):
    scores = jnp.dot(queries, key_rows.T, preferred_element_type=jnp.float32) * scales
    row_max = lax.optimization_barrier(jnp.max(scores, axis=-1, keepdims=True))
    exponent = jnp.exp(scores - row_max)
    row_total = lax.optimization_barrier(jnp.sum(exponent, axis=-1, keepdims=True))
    weights = exponent.astype(jnp.bfloat16)
    summed = jnp.dot(weights, value_rows, preferred_element_type=jnp.float32)
    return (summed / row_total).astype(jnp.bfloat16)

def reference(target, source, target_gain, source_gain, query_w, key_w, value_w, out_w, head_temp, final_gain):
    unit_source = unit_rows(source)
    group_size = HEADS // KV_HEADS
    head_share = HEADS // N_TP
    hidden_state = target.astype(jnp.float32)
    for layer_index in range(2):
        normed_source = (unit_source * source_gain[layer_index].astype(jnp.float32)).astype(jnp.bfloat16)
        key_rows = jnp.dot(normed_source, key_w[layer_index], preferred_element_type=jnp.float32).astype(jnp.bfloat16)
        value_rows = jnp.dot(normed_source, value_w[layer_index], preferred_element_type=jnp.float32).astype(jnp.bfloat16)
        key_rows = key_rows.reshape(SOURCE, KV_HEADS, HEAD_DIM)
        value_rows = value_rows.reshape(SOURCE, KV_HEADS, HEAD_DIM)
        normed = (unit_rows(hidden_state) * target_gain[layer_index].astype(jnp.float32)).astype(jnp.bfloat16)
        queries = jnp.dot(normed, query_w[layer_index], preferred_element_type=jnp.float32).astype(jnp.bfloat16)
        queries = queries.reshape(TARGET, HEADS, HEAD_DIM)
        scales = head_temp[layer_index].astype(jnp.float32) * HEAD_DIM ** (-0.5)

        def one_head(head_index):
            shared_head = head_index // group_size
            return attend_head(queries[:, head_index], key_rows[:, shared_head], value_rows[:, shared_head], scales[head_index])
        heads_out = lax.map(one_head, jnp.arange(HEADS, dtype=jnp.int32))
        heads_out = heads_out.reshape(N_TP, head_share, TARGET, HEAD_DIM)
        out_parts = out_w[layer_index].reshape(N_TP, head_share, HEAD_DIM, D)

        def part_term(running, inputs):
            head_block, weights = inputs
            partial_value = jnp.einsum('htd,hde->te', head_block.astype(jnp.float32), weights.astype(jnp.float32))
            rounded = lax.optimization_barrier(partial_value.astype(jnp.bfloat16))
            return (running + rounded.astype(jnp.float32), None)
        mixed, unused = lax.scan(part_term, jnp.zeros((TARGET, D), jnp.float32), (heads_out, out_parts))
        hidden_state = hidden_state + mixed
    return unit_rows(hidden_state) * final_gain.astype(jnp.float32)
```

```python
import jax
import jax.numpy as jnp
from jax import lax
from jax.experimental import pallas as pl
from jax.experimental.pallas import tpu as pltpu
from jax.sharding import PartitionSpec as P

HEAD_DIM = 512
EPS = 1e-06
LOG2E = 1.4426950408889634
AXES = ("sp", "tp")
VMEM_BYTES = 60 * 1024 * 1024


def unit_rows(matrix):
    values = matrix.astype(jnp.float32)
    return values * lax.rsqrt(jnp.mean(values * values, axis=-1, keepdims=True) + EPS)


def kv_project(pieces, gain, key_w, value_w, block=256):
    depth = pieces[0].shape[1]
    width = key_w.shape[1]
    count = len(pieces)
    rows = sum(piece.shape[0] for piece in pieces)
    block = min(block, width)

    def body(*refs):
        piece_refs = refs[:count]
        gain_ref, kw_ref, vw_ref, key_ref, value_ref, normed_ref = refs[count:]

        @pl.when(pl.program_id(0) == 0)
        def _():
            at = 0
            for piece_ref in piece_refs:
                size = piece_ref.shape[0]
                normed_ref[at : at + size, :] = (
                    piece_ref[...].astype(jnp.float32) * gain_ref[...]
                ).astype(jnp.bfloat16)
                at += size

        normed = normed_ref[...]
        key_ref[...] = jnp.dot(
            normed, kw_ref[...], preferred_element_type=jnp.float32
        ).astype(jnp.bfloat16)
        value_ref[...] = jnp.dot(
            normed, vw_ref[...], preferred_element_type=jnp.float32
        ).astype(jnp.bfloat16)

    return pl.pallas_call(
        body,
        grid=(width // block,),
        in_specs=[pl.BlockSpec(piece.shape, lambda j: (0, 0)) for piece in pieces]
        + [
            pl.BlockSpec((1, depth), lambda j: (0, 0)),
            pl.BlockSpec((depth, block), lambda j: (0, j)),
            pl.BlockSpec((depth, block), lambda j: (0, j)),
        ],
        out_specs=[pl.BlockSpec((rows, block), lambda j: (0, j))] * 2,
        out_shape=[jax.ShapeDtypeStruct((rows, width), jnp.bfloat16)] * 2,
        scratch_shapes=[pltpu.VMEM((rows, depth), jnp.bfloat16)],
        compiler_params=pltpu.CompilerParams(vmem_limit_bytes=VMEM_BYTES),
        cost_estimate=pl.CostEstimate(
            flops=4 * rows * depth * width,
            bytes_accessed=2 * (rows * depth + 2 * depth * width + 2 * rows * width),
            transcendentals=0,
        ),
        name="kv_project",
    )(*pieces, gain, key_w, value_w)


def attend(queries, keys, values, scales, key_block=1024):
    rows = queries.shape[0]
    heads = queries.shape[1] // HEAD_DIM
    shared = keys[0].shape[1] // HEAD_DIM
    group = heads // shared
    count = len(keys)
    total = sum(key.shape[0] for key in keys)
    blocks = []
    at = 0
    for index, key in enumerate(keys):
        size = min(key_block, key.shape[0])
        for start in range(0, key.shape[0], size):
            blocks.append((index, start, size, at))
            at += size

    def body(scale_ref, query_ref, *refs):
        key_refs, value_refs = refs[:count], refs[count : 2 * count]
        out_ref, score_ref = refs[2 * count :]
        which = pl.program_id(0)
        stacked = jnp.concatenate(
            [query_ref[:, g * HEAD_DIM : (g + 1) * HEAD_DIM] for g in range(group)], axis=0
        )
        top = None
        for index, start, size, offset in blocks:
            scores = lax.dot_general(
                stacked,
                key_refs[index][start : start + size, :],
                (((1,), (1,)), ((), ())),
                preferred_element_type=jnp.float32,
            )
            score_ref[:, offset : offset + size] = scores
            block_top = jnp.max(scores, axis=-1, keepdims=True)
            top = block_top if top is None else jnp.maximum(top, block_top)
        factor = jnp.concatenate(
            [jnp.full((rows, 1), scale_ref[which * group + g], jnp.float32) for g in range(group)],
            axis=0,
        )
        acc = None
        total_row = None
        for index, start, size, offset in blocks:
            expo = jnp.exp2((score_ref[:, offset : offset + size] - top) * factor)
            part = jnp.sum(expo, axis=-1, keepdims=True)
            total_row = part if total_row is None else total_row + part
            term = jnp.dot(
                expo.astype(jnp.bfloat16),
                value_refs[index][start : start + size, :],
                preferred_element_type=jnp.float32,
            )
            acc = term if acc is None else acc + term
        attended = (acc / total_row).astype(jnp.bfloat16)
        for g in range(group):
            out_ref[:, g * HEAD_DIM : (g + 1) * HEAD_DIM] = attended[g * rows : (g + 1) * rows]

    return pl.pallas_call(
        body,
        grid=(shared,),
        in_specs=[
            pl.BlockSpec(memory_space=pltpu.SMEM),
            pl.BlockSpec((rows, group * HEAD_DIM), lambda h: (0, h)),
        ]
        + [pl.BlockSpec((key.shape[0], HEAD_DIM), lambda h: (0, h)) for key in keys] * 2,
        out_specs=pl.BlockSpec((rows, group * HEAD_DIM), lambda h: (0, h)),
        out_shape=jax.ShapeDtypeStruct(queries.shape, jnp.bfloat16),
        scratch_shapes=[pltpu.VMEM((group * rows, total), jnp.float32)],
        compiler_params=pltpu.CompilerParams(vmem_limit_bytes=VMEM_BYTES),
        cost_estimate=pl.CostEstimate(
            flops=4 * rows * heads * HEAD_DIM * total,
            bytes_accessed=4 * (queries.size + total * shared * HEAD_DIM),
            transcendentals=rows * heads * total,
        ),
        name="attend",
    )(scales, queries, *keys, *values)


def solution(mesh):
    n_sp, n_tp = mesh.shape["sp"], mesh.shape["tp"]
    devices = n_sp * n_tp

    def swap(value, mask):
        return lax.ppermute(value, AXES, [(i, i ^ mask) for i in range(devices)])

    core = 1
    tp_masks = [1 << b for b in range(1, n_tp.bit_length() - 1)]
    sp_masks = [n_tp << b for b in range(n_sp.bit_length() - 1)]
    x_mask, y_mask = tp_masks[0], sp_masks[0]
    far_masks = (sp_masks[1:] + tp_masks[1:])[::-1]

    def plane_pieces(block):
        half = block.shape[0] // 2
        over_x = swap(block, x_mask)
        over_y = swap(block, y_mask)
        diagonal = [swap(over_y[:half], x_mask), swap(over_x[half:], y_mask)]
        mine = [block, over_x, over_y] + diagonal
        return [piece for part in mine for piece in (part, swap(part, core))]

    def per_device(
        target, source, target_gain, source_gain, query_w, key_w, value_w, out_w, head_temp,
        final_gain,
    ):
        source_unit = unit_rows(source).astype(jnp.bfloat16)
        blocks = [source_unit]
        for mask in far_masks:
            blocks = blocks + [swap(block, mask) for block in blocks]
        planes = [plane_pieces(block) for block in blocks]
        gains = source_gain.astype(jnp.float32)
        scales = head_temp * (HEAD_DIM**-0.5 * LOG2E)
        hidden_state = target.astype(jnp.float32)
        own = target.shape[0]
        for layer in range(2):
            projected = [
                kv_project(plane, gains[layer][None, :], key_w[layer], value_w[layer])
                for plane in planes
            ]
            normed = (unit_rows(hidden_state) * target_gain[layer].astype(jnp.float32)).astype(
                jnp.bfloat16
            )
            rows = [normed]
            for mask in tp_masks:
                rows = rows + [swap(row, mask) for row in rows]
            rows = [piece for row in rows for piece in (row, swap(row, core))]
            queries = jnp.dot(
                jnp.concatenate(rows, axis=0), query_w[layer], preferred_element_type=jnp.float32
            ).astype(jnp.bfloat16)
            attended = attend(
                queries, [pair[0] for pair in projected], [pair[1] for pair in projected],
                scales[layer],
            )
            partial = jnp.dot(
                attended, out_w[layer], preferred_element_type=jnp.float32
            ).astype(jnp.bfloat16)
            parts = [partial[i * own : (i + 1) * own] for i in range(n_tp)]
            received = swap(jnp.concatenate(parts[1::2], axis=0), core)
            parts = [
                part.astype(jnp.float32) + received[i * own : (i + 1) * own].astype(jnp.float32)
                for i, part in enumerate(parts[0::2])
            ]
            for mask in tp_masks[::-1]:
                keep = len(parts) // 2
                sent = jnp.concatenate(parts[keep:], axis=0).astype(jnp.bfloat16)
                received = swap(sent, mask).astype(jnp.float32)
                parts = [
                    part + received[i * own : (i + 1) * own] for i, part in enumerate(parts[:keep])
                ]
            hidden_state = hidden_state + parts[0]
        return unit_rows(hidden_state) * final_gain.astype(jnp.float32)

    in_specs = (
        P(AXES, None), P(AXES, None), P(), P(), P(None, None, "tp"), P(None, None, "tp"),
        P(None, None, "tp"), P(None, "tp", None), P(None, "tp"), P(),
    )
    return jax.shard_map(
        per_device, mesh=mesh, in_specs=in_specs, out_specs=P(AXES, None), check_vma=False
    )
```

```python
import jax
import jax.numpy as jnp
from jax import lax
from jax.experimental import pallas as pl
from jax.experimental.pallas import tpu as pltpu
from jax.sharding import PartitionSpec as P

HEAD_DIM = 512
EPS = 1e-06
LOG2E = 1.4426950408889634
AXES = ("sp", "tp")
VMEM_BYTES = 60 * 1024 * 1024


def unit_rows(matrix):
    values = matrix.astype(jnp.float32)
    return values * lax.rsqrt(jnp.mean(values * values, axis=-1, keepdims=True) + EPS)


def kv_project(pieces, gains, key_w, value_w, first, layers, after, block=256):
    depth = pieces[0].shape[1]
    width = key_w.shape[2]
    count = len(pieces)
    rows = sum(piece.shape[0] for piece in pieces)
    block = min(block, width)

    def body(*refs):
        piece_refs = refs[:count]
        gain_ref, kw_ref, vw_ref, _, key_ref, value_ref, normed_ref = refs[count:]

        @pl.when(pl.program_id(1) == 0)
        def _():
            gain = gain_ref[pl.ds(pl.program_id(0) + first, 1), :]
            at = 0
            for piece_ref in piece_refs:
                size = piece_ref.shape[0]
                normed_ref[at : at + size, :] = (
                    piece_ref[...].astype(jnp.float32) * gain
                ).astype(jnp.bfloat16)
                at += size

        normed = normed_ref[...]
        key_ref[...] = jnp.dot(
            normed, kw_ref[...], preferred_element_type=jnp.float32
        ).astype(jnp.bfloat16)
        value_ref[...] = jnp.dot(
            normed, vw_ref[...], preferred_element_type=jnp.float32
        ).astype(jnp.bfloat16)

    weight_spec = pl.BlockSpec((None, depth, block), lambda l, j: (l + first, 0, j))
    return pl.pallas_call(
        body,
        grid=(layers, width // block),
        in_specs=[pl.BlockSpec(piece.shape, lambda l, j: (0, 0)) for piece in pieces]
        + [
            pl.BlockSpec(gains.shape, lambda l, j: (0, 0)),
            weight_spec,
            weight_spec,
            pl.BlockSpec(memory_space=pl.ANY),
        ],
        out_specs=[pl.BlockSpec((None, rows, block), lambda l, j: (l, 0, j))] * 2,
        out_shape=[jax.ShapeDtypeStruct((layers, rows, width), jnp.bfloat16)] * 2,
        scratch_shapes=[pltpu.VMEM((rows, depth), jnp.bfloat16)],
        compiler_params=pltpu.CompilerParams(vmem_limit_bytes=VMEM_BYTES),
        cost_estimate=pl.CostEstimate(
            flops=4 * layers * rows * depth * width,
            bytes_accessed=2 * (rows * depth + 2 * layers * (depth + rows) * width),
            transcendentals=0,
        ),
        name="kv_project",
    )(*pieces, gains, key_w, value_w, after)


def layer_terms(row_pieces, query_w, keys, values, out_w, scales, layer, after, key_block=1024):
    count_rows = len(row_pieces)
    rows = sum(piece.shape[0] for piece in row_pieces)
    depth = query_w.shape[1]
    heads = query_w.shape[2] // HEAD_DIM
    shared = keys[0][0].shape[2] // HEAD_DIM
    group = heads // shared
    span = group * HEAD_DIM
    count = len(keys)
    sizes = [key.shape[1] for key, _ in keys]
    slots = [slot for _, slot in keys]
    starts = [sum(sizes[:i]) for i in range(count)]
    total = sum(sizes)
    key_block = min(key_block, total)
    width = out_w.shape[2]

    def body(scale_ref, *refs):
        piece_refs = refs[:count_rows]
        qw_hbm, ow_hbm = refs[count_rows : count_rows + 2]
        key_hbm = refs[count_rows + 2 : count_rows + 2 + count]
        value_hbm = refs[count_rows + 2 + count : count_rows + 2 + 2 * count]
        (_, out_ref, qw_ref, key_ref, value_ref, ow_ref, score_ref, stack_ref, acc_ref, sems) = refs[
            count_rows + 2 + 2 * count :
        ]

        copies = []
        for h in range(shared):
            group_copies = [
                [
                    pltpu.make_async_copy(
                        qw_hbm.at[layer, :, pl.ds(h * span, span)], qw_ref.at[h], sems.at[h, 0]
                    )
                ]
            ]
            for which, (sources, target_ref) in enumerate(
                ((key_hbm, key_ref), (value_hbm, value_ref))
            ):
                group_copies.append(
                    [
                        pltpu.make_async_copy(
                            sources[i].at[slots[i], :, pl.ds(h * HEAD_DIM, HEAD_DIM)],
                            target_ref.at[h, pl.ds(starts[i], sizes[i]), :],
                            sems.at[h, 3 + which * count + i],
                        )
                        for i in range(count)
                    ]
                )
            group_copies.append(
                [
                    pltpu.make_async_copy(
                        ow_hbm.at[layer, pl.ds(h * span, span), :], ow_ref.at[h], sems.at[h, 1]
                    )
                ]
            )
            copies.append(group_copies)
        for group_copies in copies:
            for batch in group_copies:
                for copy in batch:
                    copy.start()
        normed = jnp.concatenate([piece_ref[...] for piece_ref in piece_refs], axis=0)
        for h in range(shared):
            query_copy, key_copies, value_copies, out_copy = copies[h]
            query_copy[0].wait()
            queries = jnp.dot(normed, qw_ref[h], preferred_element_type=jnp.float32).astype(
                jnp.bfloat16
            )
            for g in range(group):
                stack_ref[g * rows : (g + 1) * rows, :] = queries[
                    :, g * HEAD_DIM : (g + 1) * HEAD_DIM
                ]
            for copy in key_copies:
                copy.wait()
            stacked = stack_ref[...]
            top = None
            for at in range(0, total, key_block):
                scores = lax.dot_general(
                    stacked,
                    key_ref[h, at : at + key_block, :],
                    (((1,), (1,)), ((), ())),
                    preferred_element_type=jnp.float32,
                )
                score_ref[:, at : at + key_block] = scores
                block_top = jnp.max(scores, axis=-1, keepdims=True)
                top = block_top if top is None else jnp.maximum(top, block_top)
            factor = jnp.concatenate(
                [
                    jnp.full((rows, 1), scale_ref[layer, h * group + g], jnp.float32)
                    for g in range(group)
                ],
                axis=0,
            )
            for copy in value_copies:
                copy.wait()
            acc = None
            total_row = None
            for at in range(0, total, key_block):
                expo = jnp.exp2((score_ref[:, at : at + key_block] - top) * factor)
                part = jnp.sum(expo, axis=-1, keepdims=True)
                total_row = part if total_row is None else total_row + part
                term = jnp.dot(
                    expo.astype(jnp.bfloat16),
                    value_ref[h, at : at + key_block, :],
                    preferred_element_type=jnp.float32,
                )
                acc = term if acc is None else acc + term
            attended = (acc / total_row).astype(jnp.bfloat16)
            flat = jnp.concatenate(
                [attended[g * rows : (g + 1) * rows] for g in range(group)], axis=1
            )
            out_copy[0].wait()
            term = jnp.dot(flat, ow_ref[h], preferred_element_type=jnp.float32)
            if h == 0 and shared > 1:
                acc_ref[...] = term
            elif h < shared - 1:
                acc_ref[...] += term
            elif shared > 1:
                out_ref[...] = (acc_ref[...] + term).astype(jnp.bfloat16)
            else:
                out_ref[...] = term.astype(jnp.bfloat16)

    whole = pl.BlockSpec(memory_space=pltpu.VMEM)
    hbm = pl.BlockSpec(memory_space=pl.ANY)
    return pl.pallas_call(
        body,
        in_specs=[pl.BlockSpec(memory_space=pltpu.SMEM)]
        + [whole] * count_rows
        + [hbm] * (3 + 2 * count),
        out_specs=whole,
        out_shape=jax.ShapeDtypeStruct((rows, width), jnp.bfloat16),
        scratch_shapes=[
            pltpu.VMEM((shared, depth, span), jnp.bfloat16),
            pltpu.VMEM((shared, total, HEAD_DIM), jnp.bfloat16),
            pltpu.VMEM((shared, total, HEAD_DIM), jnp.bfloat16),
            pltpu.VMEM((shared, span, width), jnp.bfloat16),
            pltpu.VMEM((group * rows, total), jnp.float32),
            pltpu.VMEM((group * rows, HEAD_DIM), jnp.bfloat16),
            pltpu.VMEM((rows, width), jnp.float32),
            pltpu.SemaphoreType.DMA((shared, 3 + 2 * count)),
        ],
        compiler_params=pltpu.CompilerParams(vmem_limit_bytes=VMEM_BYTES),
        cost_estimate=pl.CostEstimate(
            flops=4 * rows * heads * HEAD_DIM * (total + depth),
            bytes_accessed=4 * (depth * heads + total * shared) * HEAD_DIM,
            transcendentals=rows * heads * total,
        ),
        name="layer_terms",
    )(
        scales, *row_pieces, query_w, out_w, *[key for key, _ in keys],
        *[value for value, _ in values], after,
    )


def solution(mesh):
    n_sp, n_tp = mesh.shape["sp"], mesh.shape["tp"]
    devices = n_sp * n_tp

    def swap(value, mask):
        return lax.ppermute(value, AXES, [(i, i ^ mask) for i in range(devices)])

    core = 1
    tp_masks = [1 << b for b in range(1, n_tp.bit_length() - 1)]
    sp_masks = [n_tp << b for b in range(n_sp.bit_length() - 1)]
    x_mask, y_mask = tp_masks[0], sp_masks[0]
    far_masks = (sp_masks[1:] + tp_masks[1:])[::-1]

    def both_cores(block):
        return [block, swap(block, core)]

    def per_device(
        target, source, target_gain, source_gain, query_w, key_w, value_w, out_w, head_temp,
        final_gain,
    ):
        source_unit = unit_rows(source).astype(jnp.bfloat16)
        blocks = [source_unit]
        for mask in far_masks:
            blocks = blocks + [swap(block, mask) for block in blocks]
        over_x = swap(source_unit, x_mask)
        over_y = swap(source_unit, y_mask)
        corner = swap(over_x, y_mask)
        chunks = [
            both_cores(source_unit),
            both_cores(over_x) + both_cores(over_y) + both_cores(corner),
        ]
        for i, block in enumerate(blocks[1:]):
            near, far = (y_mask, x_mask) if i % 2 == 0 else (x_mask, y_mask)
            pair = jnp.concatenate([block, swap(block, near)], axis=0)
            chunks.append(both_cores(pair) + both_cores(swap(pair, far)))
        gains = source_gain.astype(jnp.float32)
        scales = head_temp * (HEAD_DIM**-0.5 * LOG2E)
        keys, values = [[], []], [[], []]
        early = len(chunks) // 2 + 1

        def project(chunk, first, layers, after):
            key, value = kv_project(chunk, gains, key_w, value_w, first, layers, after)
            for slot in range(layers):
                keys[first + slot].append((key, slot))
                values[first + slot].append((value, slot))
            return key

        after = gains
        for chunk in chunks[:early]:
            after = project(chunk, 0, 2, after)
        for chunk in chunks[early:]:
            after = project(chunk, 0, 1, after)

        hidden_state = target.astype(jnp.float32)
        own = target.shape[0]
        for layer in range(2):
            normed = (unit_rows(hidden_state) * target_gain[layer].astype(jnp.float32)).astype(
                jnp.bfloat16
            )
            rows = [normed]
            for mask in tp_masks:
                rows = rows + [swap(row, mask) for row in rows]
            rows = [piece for row in rows for piece in both_cores(row)]
            partial = layer_terms(
                rows, query_w, keys[layer], values[layer], out_w, scales, layer, after
            )
            after = partial
            if layer == 0:
                for chunk in chunks[early:]:
                    after = project(chunk, 1, 1, after)
            parts = [partial[i * own : (i + 1) * own] for i in range(n_tp)]
            received = swap(jnp.concatenate(parts[1::2], axis=0), core)
            parts = [
                part.astype(jnp.float32) + received[i * own : (i + 1) * own].astype(jnp.float32)
                for i, part in enumerate(parts[0::2])
            ]
            for mask in tp_masks[::-1]:
                keep = len(parts) // 2
                sent = jnp.concatenate(parts[keep:], axis=0).astype(jnp.bfloat16)
                received = swap(sent, mask).astype(jnp.float32)
                parts = [
                    part + received[i * own : (i + 1) * own] for i, part in enumerate(parts[:keep])
                ]
            hidden_state = hidden_state + parts[0]
        return unit_rows(hidden_state) * final_gain.astype(jnp.float32)

    in_specs = (
        P(AXES, None), P(AXES, None), P(), P(), P(None, None, "tp"), P(None, None, "tp"),
        P(None, None, "tp"), P(None, "tp", None), P(None, "tp"), P(),
    )
    return jax.shard_map(
        per_device, mesh=mesh, in_specs=in_specs, out_specs=P(AXES, None), check_vma=False
    )
```
